32 devices in a mesh: sp: 8 (over z, x), tp: 4 (over y, core).
Axes of the slice: x: 2, y: 2, z: 4, core: 2. Of those that a mesh axis runs over, the one named last changes fastest.
Arguments:
- tokens: bfloat16 [4096, 4096], P('sp', 'tp'), may hold values from -8 to 8
- w_key: bfloat16 [4096, 2048], P(None, 'tp'), may hold values from -0.09375 to 0.09375
- w_value: bfloat16 [4096, 2048], P(None, 'tp'), may hold values from -0.09375 to 0.09375
- w_beta: bfloat16 [4096, 16], replicated, may hold values from -0.09375 to 0.09375
- w_decay: bfloat16 [4096, 16], replicated, may hold values from -0.09375 to 0.09375
- beta_bias: float32 [16], replicated, may hold values from -6 to -4
- decay_rate: float32 [16], replicated, as said below
- forgetting_increment: float32 [16, 4096], P('tp', 'sp')
- new_query: bfloat16 [16, 128], P('tp', 'sp'), may hold values from -6 to 6
- read_gain: bfloat16 [128], replicated, may hold values from 0.099609375 to 1.8984375
Outputs:
- state_cache: bfloat16 [16, 128, 128], P('tp', 'sp')
- first_read: float32 [16, 128], P('tp')
The draws below stay inside these ranges and needn't reach their ends.
Inputs may be any that keep to these rules, and one draw needn't show every extreme that they name: `decay_rate`: positive.
All inputs are finite; a program needn't handle non-finite values.
Results may differ from the reference program's by a relative error of at most 0.0075.
Values may be sent and summed in bfloat16 or wider, within the bound.
A program may use at most 64 MiB of HBM per device.

```python
import math
import jax
import jax.numpy as jnp
from jax import lax

D = 4096
HEADS = 16
DK = 128
DV = 128
BLOCK = 64
LENGTH = 4096


def draw_tokens(key, part):
    perturbation_seed, common_key = jax.random.split(key, 2)
    blocks = LENGTH // BLOCK
    noise = jnp.clip(jax.random.normal(perturbation_seed, (LENGTH, D), jnp.float32), -4.5, 4.5)
    common = jnp.clip(jax.random.normal(common_key, (blocks, D), jnp.float32), -4.5, 4.5)
    mixed = noise + 0.7 * jnp.repeat(common, BLOCK, axis=0)
    return mixed.astype(jnp.bfloat16)


def draw_decay_rate(key, part):
    slow_key, fast_key, pick_key = jax.random.split(key, 3)
    slow = jnp.exp(jax.random.uniform(slow_key, (HEADS,), jnp.float32, math.log(0.2 / LENGTH), math.log(1.0 / LENGTH)))
    fast = jnp.exp(jax.random.uniform(fast_key, (HEADS,), jnp.float32, math.log(0.02), math.log(0.06)))
    picked = jax.random.bernoulli(pick_key, 0.5, (HEADS,))
    return jnp.where(picked, fast, slow)


def draw_forgetting_increment(key, part):
    scale_key, location_seed, drop_key = jax.random.split(key, 3)
    blocks = LENGTH // BLOCK
    factor = jnp.exp(jax.random.uniform(scale_key, (HEADS, blocks), jnp.float32, math.log(0.25), math.log(4.0)))
    starting_displacement = -jnp.repeat(factor, BLOCK, axis=1) / LENGTH
    location_positions = jax.random.randint(location_seed, (HEADS, 4), 0, LENGTH)
    discarded_elements = jnp.log(jax.random.uniform(drop_key, (HEADS, 4), jnp.float32, 0.5, 0.8))
    breadth_across = jnp.arange(LENGTH)
    cluster_batches = jnp.sum(jnp.where(breadth_across[None, None, :] == location_positions[:, :, None], discarded_elements[:, :, None], 0.0), axis=1)
    return starting_displacement + cluster_batches


def levels(stream_key, dims, shards, least, largest):
    level, own = 1.0, jax.random.fold_in(stream_key, 6)
    for dim, shards_of in shards:
        draws = jnp.exp(jax.random.uniform(jax.random.fold_in(own, dim), (shards_of,), jnp.float32, least / len(shards), largest / len(shards)))
        level = level * jnp.repeat(draws, dims[dim] // shards_of).reshape([-1 if axis == dim else 1 for axis in range(len(dims))])
    return level


def centred(own_key, shape, scale, limit, pieces=(), kind=jnp.bfloat16):
    array = jax.random.normal(own_key, shape, jnp.float32) * scale
    if len(pieces) > 0:
        array = levels(own_key, shape, pieces, -0.22, 0.18) * array
    return jnp.clip(array, min=-limit, max=limit).astype(kind)


def setup_inputs(seed: int = 0) -> dict:
    streams_of = jax.random.split(jax.random.key(seed), 11)
    return {
        "tokens": draw_tokens(jax.random.fold_in(streams_of[10], 71), 0),
        "w_key": centred(streams_of[1], (D, HEADS * DK), D ** -0.5, 0.09375, ((1, 4),)),
        "w_value": centred(streams_of[2], (D, HEADS * DV), D ** -0.5, 0.09375, ((1, 4),)),
        "w_beta": centred(streams_of[3], (D, HEADS), D ** -0.5, 0.09375),
        "w_decay": centred(streams_of[4], (D, HEADS), D ** -0.5, 0.09375),
        "beta_bias": jnp.clip(jax.random.uniform(streams_of[5], (HEADS,), jnp.float32, -6.0, -4.0), -6.0, -4.0),
        "decay_rate": draw_decay_rate(jax.random.fold_in(streams_of[10], 71), 0),
        "forgetting_increment": draw_forgetting_increment(jax.random.fold_in(streams_of[10], 71), 0),
        "new_query": centred(streams_of[8], (HEADS, DK), 1.0, 6.0, ((0, 4), (1, 8))),
        "read_gain": jnp.clip(1.0 + 0.18 * jax.random.normal(streams_of[9], (DV,), jnp.float32), 0.099609375, 1.8984375).astype(jnp.bfloat16),
    }


norm_eps = 1e-06

def matmul_f32(left, right):
    return jnp.dot(left, right, precision=lax.Precision.HIGHEST)

def unit_inverse(lower):
    current_size = lower.shape[0]
    identity = jnp.eye(current_size, dtype=jnp.float32)
    result = identity - lower
    lower_power = lower
    covered = 2
    while covered < current_size:
        lower_power = matmul_f32(lower_power, lower_power)
        result = matmul_f32(result, identity + lower_power)
        covered = covered * 2
    return result

def block_terms(key_blk, value_blk, beta_blk, logd_blk):
    current_size = key_blk.shape[0]
    cumulative = jnp.cumsum(logd_blk)
    spread = cumulative[:, None] - cumulative[None, :]
    location_positions = jnp.arange(current_size)
    causal = location_positions[:, None] >= location_positions[None, :]
    strict = location_positions[:, None] > location_positions[None, :]
    decay_table = jnp.where(causal, jnp.exp(jnp.where(causal, spread, 0.0)), 0.0)
    key_beta = key_blk * beta_blk[:, None]
    lower = jnp.where(strict, matmul_f32(key_beta, key_blk.T) * decay_table, 0.0)
    inverse = unit_inverse(lower)
    update = matmul_f32(inverse, value_blk * beta_blk[:, None])
    erase = matmul_f32(inverse, key_beta * jnp.exp(cumulative)[:, None])
    key_remainder = key_blk * jnp.exp(cumulative[-1] - cumulative)[:, None]
    return (update, erase, key_remainder, jnp.exp(cumulative[-1]))

def reference(tokens, w_key, w_value, w_beta, w_decay, beta_bias, decay_rate, forgetting_increment, new_query, read_gain):
    key_raw = jnp.dot(tokens, w_key, preferred_element_type=jnp.float32).astype(jnp.bfloat16)
    value_raw = jnp.dot(tokens, w_value, preferred_element_type=jnp.float32).astype(jnp.bfloat16)
    key_wide = lax.optimization_barrier(key_raw).astype(jnp.float32).reshape(LENGTH, HEADS, DK)
    key_unit = key_wide * lax.rsqrt(lax.optimization_barrier(jnp.sum(key_wide * key_wide, axis=-1, keepdims=True)) + norm_eps)
    value_wide = lax.optimization_barrier(value_raw).astype(jnp.float32).reshape(LENGTH, HEADS, DV)
    beta = jax.nn.sigmoid(jnp.dot(tokens, w_beta, preferred_element_type=jnp.float32) + beta_bias)
    log_decay = -decay_rate * jax.nn.softplus(jnp.dot(tokens, w_decay, preferred_element_type=jnp.float32)) + forgetting_increment.T
    blocks = LENGTH // BLOCK
    key_heads = key_unit.transpose(1, 0, 2).reshape(HEADS, blocks, BLOCK, DK)
    value_heads = value_wide.transpose(1, 0, 2).reshape(HEADS, blocks, BLOCK, DV)
    beta_heads = beta.T.reshape(HEADS, blocks, BLOCK)
    logd_heads = log_decay.T.reshape(HEADS, blocks, BLOCK)
    terms = jax.vmap(jax.vmap(block_terms))(key_heads, value_heads, beta_heads, logd_heads)
    inputs = tuple((jnp.moveaxis(item, 1, 0) for item in terms))

    def advance(state, block_in):
        update, erase, key_remainder, keep = block_in
        fresh = update - jnp.einsum('hcd,hde->hce', erase, state, precision=lax.Precision.HIGHEST)
        state = keep[:, None, None] * state + jnp.einsum('hcd,hce->hde', key_remainder, fresh, precision=lax.Precision.HIGHEST)
        return (state, None)
    final_state, _ = lax.scan(advance, jnp.zeros((HEADS, DK, DV), jnp.float32), inputs)
    state_cache = final_state.astype(jnp.bfloat16)
    raw_read = lax.optimization_barrier(jnp.sum(new_query.astype(jnp.float32)[:, :, None] * state_cache.astype(jnp.float32), axis=1))
    first_read = raw_read * lax.rsqrt(lax.optimization_barrier(jnp.mean(raw_read * raw_read, axis=-1, keepdims=True)) + norm_eps) * read_gain.astype(jnp.float32)
    return (state_cache, first_read)
```

```python
import functools

import jax
import jax.numpy as jnp
from jax import lax
from jax.experimental import pallas as pl
from jax.experimental.pallas import tpu as pltpu
from jax.sharding import PartitionSpec as P

DK = 128
DV = 128
CHUNK = 128
LANES = 128
SUB = 8
norm_eps = 1e-06
MESH = pl.DeviceIdType.MESH
F32 = jnp.float32
BF16 = jnp.bfloat16


def mm(left, right):
    return jnp.dot(left.astype(BF16), right.astype(BF16), preferred_element_type=F32)


def mm_nt(left, right):
    return lax.dot_general(
        left.astype(BF16), right.astype(BF16), (((1,), (1,)), ((), ())), preferred_element_type=F32
    )


def log2(value):
    return value.bit_length() - 1


def body(
    n_sp,
    n_tp,
    x_ref,
    wk_hbm,
    wv_hbm,
    wb_hbm,
    wd_hbm,
    bias_ref,
    rate_ref,
    finc_ref,
    q_ref,
    gain_ref,
    state_out,
    read_out,
    wk,
    wv,
    wb,
    wd,
    wg,
    xg,
    acck,
    accv,
    accg,
    maps,
    gams,
    sendbuf,
    recvbuf,
    gsend,
    grecv,
    qslots,
    fstate,
    srecv,
    fread,
    rrecv,
    wsem,
    own_send,
    peer_send,
    fwd_send,
    tok_recv,
    q_send,
    q_recv,
    map_send,
    map_recv,
    g_send,
    g_recv,
    s_send,
    s_recv,
    r_send,
    r_recv,
):
    sp = lax.axis_index("sp")
    tp = lax.axis_index("tp")
    tokens_here, features = x_ref.shape
    heads = wk.shape[1] // DK
    chunks = tokens_here // CHUNK
    n_y = n_tp // 2
    y = tp // 2
    core = tp % 2
    sibling = tp + 1 - 2 * core
    levels = log2(n_sp)
    rows_out = DK // n_sp

    loads = [
        pltpu.make_async_copy(wk_hbm, wk, wsem.at[0]),
        pltpu.make_async_copy(wv_hbm, wv, wsem.at[1]),
        pltpu.make_async_copy(wb_hbm, wb, wsem.at[2]),
        pltpu.make_async_copy(wd_hbm, wd, wsem.at[3]),
    ]
    for load in (loads[2], loads[3], loads[0], loads[1]):
        load.start()

    barrier = pltpu.get_barrier_semaphore()
    pl.semaphore_signal(barrier, inc=1, device_id={"tp": sibling}, device_id_type=MESH)
    for step in range(1, n_y):
        peer = ((y + step) % n_y) * 2 + core
        pl.semaphore_signal(barrier, inc=1, device_id={"tp": peer}, device_id_type=MESH)
    for step in range(1, n_sp):
        pl.semaphore_signal(
            barrier, inc=1, device_id={"sp": (sp + step) % n_sp}, device_id_type=MESH
        )
    pl.semaphore_wait(barrier, n_y + n_sp - 1)

    def rows_of(c):
        return pl.ds(c * CHUNK, CHUNK)

    def copy_own(c):
        return pltpu.make_async_remote_copy(
            src_ref=x_ref.at[rows_of(c)],
            dst_ref=xg.at[tp, rows_of(c)],
            send_sem=own_send.at[c],
            recv_sem=tok_recv.at[tp, c],
            device_id={"tp": sibling},
            device_id_type=MESH,
        )

    def copy_peer(step, c):
        peer = ((y + step) % n_y) * 2 + core
        return pltpu.make_async_remote_copy(
            src_ref=x_ref.at[rows_of(c)],
            dst_ref=xg.at[tp, rows_of(c)],
            send_sem=peer_send.at[step, c],
            recv_sem=tok_recv.at[tp, c],
            device_id={"tp": peer},
            device_id_type=MESH,
        )

    def copy_forward(step, c):
        source = ((y + n_y - step) % n_y) * 2 + core
        return pltpu.make_async_remote_copy(
            src_ref=xg.at[source, rows_of(c)],
            dst_ref=xg.at[source, rows_of(c)],
            send_sem=fwd_send.at[step, c],
            recv_sem=tok_recv.at[source, c],
            device_id={"tp": sibling},
            device_id_type=MESH,
        )

    def arrived(source, c):
        pltpu.make_async_remote_copy(
            src_ref=xg.at[source, rows_of(c)],
            dst_ref=xg.at[source, rows_of(c)],
            send_sem=own_send.at[c],
            recv_sem=tok_recv.at[source, c],
            device_id={"tp": sibling},
            device_id_type=MESH,
        ).wait_recv()

    for c in range(chunks):
        for step in range(1, n_y):
            copy_peer(step, c).start()
        copy_own(c).start()

    def copy_query(step):
        return pltpu.make_async_remote_copy(
            src_ref=q_ref,
            dst_ref=qslots.at[sp],
            send_sem=q_send.at[step],
            recv_sem=q_recv.at[sp],
            device_id={"sp": (sp + step) % n_sp},
            device_id_type=MESH,
        )

    for step in range(1, n_sp):
        copy_query(step).start()

    total_heads = wb.shape[1]
    row_id = lax.broadcasted_iota(jnp.int32, (total_heads, LANES), 0)
    lane_id = lax.broadcasted_iota(jnp.int32, (total_heads, LANES), 1)
    first_head = tp * heads
    pick_b = jnp.where((row_id == lane_id + first_head) & (lane_id < heads), 1.0, 0.0)
    pick_d = jnp.where(
        (row_id == lane_id - SUB + first_head) & (lane_id >= SUB) & (lane_id < SUB + heads),
        1.0,
        0.0,
    )
    loads[2].wait()
    loads[3].wait()
    depth = wg.shape[0]
    piece = 512

    def pick(step, carry):
        rows = pl.ds(pl.multiple_of(step * piece, piece), piece)
        wg[rows, :] = (mm(wb[rows, :], pick_b) + mm(wd[rows, :], pick_d)).astype(BF16)
        return carry

    lax.fori_loop(0, depth // piece, pick, 0)
    loads[0].wait()
    loads[1].wait()

    def project(x, source, rows, first=False):
        deep = pl.ds(pl.multiple_of(source * features, features), features)
        for acc, weights in ((acck, wk), (accv, wv), (accg, wg)):
            part = jnp.dot(x, weights[deep, :], preferred_element_type=F32)
            acc[rows, :] = part if first else acc[rows, :] + part

    half_rows = 256 if tokens_here % 256 == 0 else CHUNK

    def own_project(step, carry):
        rows = pl.ds(pl.multiple_of(step * half_rows, half_rows), half_rows)
        project(x_ref[rows, :], tp, rows, True)
        return carry

    lax.fori_loop(0, tokens_here // half_rows, own_project, 0)
    for c in range(chunks):
        arrived(sibling, c)

    def sibling_project(step, carry):
        rows = pl.ds(pl.multiple_of(step * half_rows, half_rows), half_rows)
        project(xg[sibling, rows, :], sibling, rows)
        return carry

    lax.fori_loop(0, tokens_here // half_rows, sibling_project, 0)

    row8 = lax.broadcasted_iota(jnp.int32, (SUB, total_heads), 0)
    lane8 = lax.broadcasted_iota(jnp.int32, (SUB, total_heads), 1)
    mine = (lane8 == row8 + first_head) & (row8 < heads)
    bias_col = jnp.sum(jnp.where(mine, bias_ref[...], 0.0), axis=1, keepdims=True)
    rate_col = jnp.sum(jnp.where(mine, rate_ref[...], 0.0), axis=1, keepdims=True)

    maps[...] = jnp.zeros_like(maps)
    gams[...] = jnp.ones_like(gams)

    def chunk_step(c, carry):
        rows = pl.ds(pl.multiple_of(c * CHUNK, CHUNK), CHUNK)
        for step in range(1, n_y):
            arrived(((y + n_y - step) % n_y) * 2 + core, c)
            copy_forward(step, c).start()
        for step in range(1, n_y):
            source = ((y + n_y - step) % n_y) * 2 + core
            project(xg[source, rows, :], source, rows)
        for step in range(1, n_y):
            source = ((y + n_y - step) % n_y) * 2 + 1 - core
            arrived(source, c)
            project(xg[source, rows, :], source, rows)

        ri = lax.broadcasted_iota(jnp.int32, (CHUNK, CHUNK), 0)
        ci = lax.broadcasted_iota(jnp.int32, (CHUNK, CHUNK), 1)
        strict = ri > ci
        upper = jnp.where(ri <= ci, 1.0, 0.0)
        gates = jnp.transpose(accg[rows, :])
        beta = jax.nn.sigmoid(gates[0:SUB, :] + bias_col)
        raw = gates[SUB : 2 * SUB, :]
        softplus = jnp.maximum(raw, 0.0) + jnp.log1p(jnp.exp(-jnp.abs(raw)))
        logd = -rate_col * softplus + finc_ref[:, rows]
        cum = jnp.dot(logd, upper, precision=lax.Precision.HIGHEST, preferred_element_type=F32)
        total = jnp.sum(logd, axis=1, keepdims=True)
        columns = jnp.transpose(
            jnp.concatenate(
                [
                    beta,
                    cum,
                    jnp.exp(cum),
                    jnp.exp(total - cum),
                    jnp.zeros((LANES - 4 * SUB, LANES), F32),
                ],
                axis=0,
            )
        )
        keep = jnp.exp(total)

        keys, rights, powers, remains = [], [], [], []
        for h in range(heads):
            cols = slice(h * DK, (h + 1) * DK)
            key = acck[rows, cols].astype(BF16).astype(F32)
            key = key * lax.rsqrt(jnp.sum(key * key, axis=-1, keepdims=True) + norm_eps)
            value = accv[rows, cols].astype(BF16).astype(F32)
            b_col = columns[:, h : h + 1]
            c_col = columns[:, SUB + h : SUB + h + 1]
            e_col = columns[:, 2 * SUB + h : 2 * SUB + h + 1]
            r_col = columns[:, 3 * SUB + h : 3 * SUB + h + 1]
            key_beta = key * b_col
            decay = jnp.exp(jnp.where(strict, c_col - cum[h : h + 1, :], 0.0))
            powers.append(jnp.where(strict, mm_nt(key_beta, key) * decay, 0.0))
            rights.append(jnp.concatenate([value * b_col, key_beta * e_col], axis=1))
            remains.append(jnp.transpose(key * r_col))
        solved = [rights[h] - mm(powers[h], rights[h]) for h in range(heads)]
        covered = 2
        while covered < CHUNK:
            powers = [mm(power, power) for power in powers]
            solved = [solved[h] + mm(powers[h], solved[h]) for h in range(heads)]
            covered *= 2
        fresh = []
        for h in range(heads):
            gamma = gams[h, 0:1, 0:1]
            erase = solved[h][:, DV:]
            direct = jnp.concatenate([solved[h][:, :DV], -gamma * erase], axis=1)
            fresh.append(direct - mm(erase, maps[h]))
        for h in range(heads):
            maps[h] = keep[h : h + 1, :] * maps[h] + mm(remains[h], fresh[h])
            gams[h] = keep[h : h + 1, :] * gams[h]
        return carry

    lax.fori_loop(0, chunks, chunk_step, 0)

    count = heads
    offset = 0
    my_head = 0
    for level in range(levels):
        bit = (sp // (1 << level)) % 2
        partner = sp + (1 - 2 * bit) * (1 << level)
        split = count > 1
        half = count // 2 if split else count
        keep_at = my_head + (bit * half if split else 0)
        send_at = my_head + ((1 - bit) * half if split else 0)
        rows = pl.ds(offset, half)
        for i in range(half):
            sendbuf[offset + i] = maps[send_at + i].astype(BF16)
            gsend[offset + i] = gams[send_at + i]
        move = pltpu.make_async_remote_copy(
            src_ref=sendbuf.at[rows],
            dst_ref=recvbuf.at[rows],
            send_sem=map_send.at[level],
            recv_sem=map_recv.at[level],
            device_id={"sp": partner},
            device_id_type=MESH,
        )
        move_g = pltpu.make_async_remote_copy(
            src_ref=gsend.at[rows],
            dst_ref=grecv.at[rows],
            send_sem=g_send.at[level],
            recv_sem=g_recv.at[level],
            device_id={"sp": partner},
            device_id_type=MESH,
        )
        move.start()
        move_g.start()
        move.wait()
        move_g.wait()
        later = bit == 1
        for i in range(half):
            own = maps[keep_at + i]
            if not split:
                own = own.astype(BF16).astype(F32)
            own_g = gams[keep_at + i]
            got = recvbuf[offset + i].astype(F32)
            got_g = grecv[offset + i]
            left = jnp.where(later, own, got)
            left_g = jnp.where(later, own_g, got_g)
            right = jnp.where(later, got, own)
            right_g = jnp.where(later, got_g, own_g)
            tail = left[:, DV:]
            added = jnp.concatenate([left[:, :DV], right_g[0:1, 0:1] * tail], axis=1)
            maps[keep_at + i] = left_g[0:1, 0:1] * right + mm(tail, right) + added
            gams[keep_at + i] = left_g * right_g
        offset += half
        count = half
        my_head = keep_at

    final = maps[my_head][:, :DV]
    for j in range(n_sp):
        fstate[j] = final[j * rows_out : (j + 1) * rows_out, :].astype(BF16)

    member = sp % heads
    base = sp - member

    def head_of(index):
        found = 0
        for place in range(log2(heads)):
            found = found * 2 + (index // (1 << place)) % 2
        return found

    def copy_state(step):
        target = base + (member + step) % heads
        return pltpu.make_async_remote_copy(
            src_ref=fstate.at[target],
            dst_ref=srecv.at[my_head],
            send_sem=s_send.at[step],
            recv_sem=s_recv.at[my_head],
            device_id={"sp": target},
            device_id_type=MESH,
        )

    for step in range(1, heads):
        copy_state(step).start()
    srecv[my_head] = fstate[sp]

    for step in range(1, n_sp):
        source = (sp + n_sp - step) % n_sp
        pltpu.make_async_remote_copy(
            src_ref=q_ref,
            dst_ref=qslots.at[source],
            send_sem=q_send.at[step],
            recv_sem=q_recv.at[source],
            device_id={"sp": source},
            device_id_type=MESH,
        ).wait_recv()
    qslots[sp] = q_ref[...]
    query = jnp.sum(qslots[...], axis=0)
    reads = mm(query, final)
    row_head = lax.broadcasted_iota(jnp.int32, (SUB, DV), 0)
    raw_read = jnp.sum(jnp.where(row_head == my_head, reads, 0.0), axis=0, keepdims=True)
    read = (
        raw_read
        * lax.rsqrt(jnp.mean(raw_read * raw_read, axis=-1, keepdims=True) + norm_eps)
        * gain_ref[...].astype(F32)
    )
    fread[...] = jnp.broadcast_to(read, fread.shape)

    def copy_read(step):
        target = base + (member + step) % heads
        return pltpu.make_async_remote_copy(
            src_ref=fread,
            dst_ref=rrecv.at[my_head],
            send_sem=r_send.at[step],
            recv_sem=r_recv.at[my_head],
            device_id={"sp": target},
            device_id_type=MESH,
        )

    for step in range(1, heads):
        copy_read(step).start()
    rrecv[my_head] = fread[...]

    for step in range(1, heads):
        other = (member + heads - step) % heads
        source = base + other
        head = head_of(other)
        pltpu.make_async_remote_copy(
            src_ref=fstate.at[source],
            dst_ref=srecv.at[head],
            send_sem=s_send.at[step],
            recv_sem=s_recv.at[head],
            device_id={"sp": source},
            device_id_type=MESH,
        ).wait_recv()
        pltpu.make_async_remote_copy(
            src_ref=fread,
            dst_ref=rrecv.at[head],
            send_sem=r_send.at[step],
            recv_sem=r_recv.at[head],
            device_id={"sp": source},
            device_id_type=MESH,
        ).wait_recv()
    for h in range(heads):
        state_out[h] = srecv[h]
        read_out[h : h + 1, :] = rrecv[h, 0:1, :]

    for c in range(chunks):
        copy_own(c).wait_send()
        for step in range(1, n_y):
            copy_peer(step, c).wait_send()
            copy_forward(step, c).wait_send()
    for step in range(1, n_sp):
        copy_query(step).wait_send()
    for step in range(1, heads):
        copy_state(step).wait_send()
        copy_read(step).wait_send()


def per_device(
    n_sp,
    n_tp,
    tokens,
    w_key,
    w_value,
    w_beta,
    w_decay,
    beta_bias,
    decay_rate,
    forgetting_increment,
    new_query,
    read_gain,
):
    tokens_here, features = tokens.shape
    depth, width = w_key.shape
    heads = width // DK
    chunks = tokens_here // CHUNK
    rows_out = DK // n_sp
    n_y = n_tp // 2
    levels = log2(n_sp)
    slots = 0
    count = heads
    for _ in range(levels):
        count = max(count // 2, 1)
        slots += count
    query = lax.dynamic_update_slice(
        jnp.zeros((SUB, DK), F32),
        new_query.astype(F32),
        (0, lax.axis_index("sp") * rows_out),
    )
    increments = jnp.pad(forgetting_increment, ((0, SUB - heads), (0, 0)))
    vmem = pl.BlockSpec(memory_space=pltpu.VMEM)
    hbm = pl.BlockSpec(memory_space=pl.ANY)
    dma = pltpu.SemaphoreType.DMA
    return pl.pallas_call(
        functools.partial(body, n_sp, n_tp),
        name="delta_state",
        out_shape=(
            jax.ShapeDtypeStruct((heads, rows_out, DV), BF16),
            jax.ShapeDtypeStruct((heads, DV), F32),
        ),
        in_specs=[vmem, hbm, hbm, hbm, hbm, vmem, vmem, vmem, vmem, vmem],
        out_specs=(vmem, vmem),
        scratch_shapes=[
            pltpu.VMEM((depth, width), BF16),
            pltpu.VMEM((depth, width), BF16),
            pltpu.VMEM(w_beta.shape, BF16),
            pltpu.VMEM(w_decay.shape, BF16),
            pltpu.VMEM((depth, LANES), BF16),
            pltpu.VMEM((n_tp, tokens_here, features), BF16),
            pltpu.VMEM((tokens_here, width), F32),
            pltpu.VMEM((tokens_here, width), F32),
            pltpu.VMEM((tokens_here, LANES), F32),
            pltpu.VMEM((heads, DK, DV + DK), F32),
            pltpu.VMEM((heads, SUB, LANES), F32),
            pltpu.VMEM((slots, DK, DV + DK), BF16),
            pltpu.VMEM((slots, DK, DV + DK), BF16),
            pltpu.VMEM((slots, SUB, LANES), F32),
            pltpu.VMEM((slots, SUB, LANES), F32),
            pltpu.VMEM((n_sp, SUB, DK), F32),
            pltpu.VMEM((n_sp, rows_out, DV), BF16),
            pltpu.VMEM((heads, rows_out, DV), BF16),
            pltpu.VMEM((SUB, DV), F32),
            pltpu.VMEM((heads, SUB, DV), F32),
            dma((4,)),
            dma((chunks,)),
            dma((n_y, chunks)),
            dma((n_y, chunks)),
            dma((n_tp, chunks)),
            dma((n_sp,)),
            dma((n_sp,)),
            dma((levels,)),
            dma((levels,)),
            dma((levels,)),
            dma((levels,)),
            dma((heads,)),
            dma((heads,)),
            dma((heads,)),
            dma((heads,)),
        ],
        compiler_params=pltpu.CompilerParams(
            collective_id=0, has_side_effects=True, vmem_limit_bytes=60 * 1024 * 1024
        ),
    )(
        tokens,
        w_key,
        w_value,
        w_beta,
        w_decay,
        beta_bias[None, :],
        decay_rate[None, :],
        increments,
        query,
        read_gain[None, :],
    )


def solution(mesh):
    return jax.shard_map(
        functools.partial(per_device, mesh.shape["sp"], mesh.shape["tp"]),
        mesh=mesh,
        in_specs=(
            P("sp", "tp"),
            P(None, "tp"),
            P(None, "tp"),
            P(),
            P(),
            P(),
            P(),
            P("tp", "sp"),
            P("tp", "sp"),
            P(),
        ),
        out_specs=(P("tp", "sp", None), P("tp", None)),
        check_vma=False,
    )
```

```python
import functools

import jax
import jax.numpy as jnp
from jax import lax
from jax.experimental import pallas as pl
from jax.experimental.pallas import tpu as pltpu
from jax.sharding import PartitionSpec as P

DK = 128
DV = 128
CHUNK = 128
LANES = 128
SUB = 8
norm_eps = 1e-06
MESH = pl.DeviceIdType.MESH
F32 = jnp.float32
BF16 = jnp.bfloat16


def mm(left, right):
    return jnp.dot(left.astype(BF16), right.astype(BF16), preferred_element_type=F32)


def mm_nt(left, right):
    return lax.dot_general(
        left.astype(BF16), right.astype(BF16), (((1,), (1,)), ((), ())), preferred_element_type=F32
    )


def log2(value):
    return value.bit_length() - 1


def tail_pieces(features):
    return 4 if features % 1024 == 0 else 1


def body(
    n_sp,
    n_tp,
    x_hbm,
    wk_hbm,
    wv_hbm,
    wb_hbm,
    wd_hbm,
    bias_ref,
    rate_ref,
    finc_ref,
    q_ref,
    gain_ref,
    state_out,
    read_out,
    wk,
    wv,
    wb,
    wd,
    wg,
    x_ref,
    finc8,
    q_own,
    xg,
    acck,
    accv,
    accg,
    maps,
    gams,
    sendbuf,
    recvbuf,
    gsend,
    grecv,
    qslots,
    fstate,
    srecv,
    fread,
    rrecv,
    wsem,
    own_send,
    peer_send,
    fwd_send,
    tok_recv,
    q_send,
    q_recv,
    map_send,
    map_recv,
    g_send,
    g_recv,
    s_send,
    s_recv,
    r_send,
    r_recv,
):
    sp = lax.axis_index("sp")
    tp = lax.axis_index("tp")
    tokens_here, features = x_ref.shape
    heads = wk.shape[1] // DK
    chunks = tokens_here // CHUNK
    last = chunks - 1
    pieces = tail_pieces(features)
    wide = features // pieces
    parts = last + pieces
    n_y = n_tp // 2
    y = tp // 2
    core = tp % 2
    sibling = tp + 1 - 2 * core
    levels = log2(n_sp)
    rows_out = DK // n_sp

    load_x = pltpu.make_async_copy(x_hbm, x_ref, wsem.at[4])
    load_x.start()
    loads = [
        pltpu.make_async_copy(wk_hbm, wk, wsem.at[0]),
        pltpu.make_async_copy(wv_hbm, wv, wsem.at[1]),
        pltpu.make_async_copy(wb_hbm, wb, wsem.at[2]),
        pltpu.make_async_copy(wd_hbm, wd, wsem.at[3]),
    ]
    for load in (loads[2], loads[3], loads[0], loads[1]):
        load.start()

    barrier = pltpu.get_barrier_semaphore()
    pl.semaphore_signal(barrier, inc=1, device_id={"tp": sibling}, device_id_type=MESH)
    for step in range(1, n_y):
        peer = ((y + step) % n_y) * 2 + core
        pl.semaphore_signal(barrier, inc=1, device_id={"tp": peer}, device_id_type=MESH)
    masks = sorted(set(range(1, heads)) | {1 << level for level in range(levels)})

    def flip(mask):
        found = sp
        for place in range(levels):
            if (mask >> place) % 2:
                found = found + (1 - 2 * ((sp // (1 << place)) % 2)) * (1 << place)
        return found

    for mask in masks:
        pl.semaphore_signal(barrier, inc=1, device_id={"sp": flip(mask)}, device_id_type=MESH)

    def part_of(k):
        if isinstance(k, int) and k >= last:
            return pl.ds(last * CHUNK, CHUNK), pl.ds((k - last) * wide, wide)
        start = k * CHUNK if isinstance(k, int) else pl.multiple_of(k * CHUNK, CHUNK)
        return pl.ds(start, CHUNK), pl.ds(0, features)

    def copy_own(k):
        rows, cols = part_of(k)
        return pltpu.make_async_remote_copy(
            src_ref=x_ref.at[rows, cols],
            dst_ref=xg.at[tp, rows, cols],
            send_sem=own_send.at[k],
            recv_sem=tok_recv.at[tp, k],
            device_id={"tp": sibling},
            device_id_type=MESH,
        )

    def copy_peer(step, k):
        rows, cols = part_of(k)
        peer = ((y + step) % n_y) * 2 + core
        return pltpu.make_async_remote_copy(
            src_ref=x_ref.at[rows, cols],
            dst_ref=xg.at[tp, rows, cols],
            send_sem=peer_send.at[step, k],
            recv_sem=tok_recv.at[tp, k],
            device_id={"tp": peer},
            device_id_type=MESH,
        )

    def copy_forward(step, k):
        rows, cols = part_of(k)
        source = ((y + n_y - step) % n_y) * 2 + core
        return pltpu.make_async_remote_copy(
            src_ref=xg.at[source, rows, cols],
            dst_ref=xg.at[source, rows, cols],
            send_sem=fwd_send.at[step, k],
            recv_sem=tok_recv.at[source, k],
            device_id={"tp": sibling},
            device_id_type=MESH,
        )

    def arrived(source, k):
        rows, cols = part_of(k)
        pltpu.make_async_remote_copy(
            src_ref=xg.at[source, rows, cols],
            dst_ref=xg.at[source, rows, cols],
            send_sem=own_send.at[k],
            recv_sem=tok_recv.at[source, k],
            device_id={"tp": sibling},
            device_id_type=MESH,
        ).wait_recv()

    pl.semaphore_wait(barrier, n_y + len(masks))
    load_x.wait()
    for k in range(parts):
        for step in range(1, n_y):
            copy_peer(step, k).start()
        copy_own(k).start()

    rows_q = lax.broadcasted_iota(jnp.int32, (rows_out, LANES), 0)
    lanes_q = lax.broadcasted_iota(jnp.int32, (rows_out, LANES), 1)
    place_q = jnp.where(lanes_q == rows_q + sp * rows_out, 1.0, 0.0)
    q_own[...] = jnp.zeros_like(q_own)
    q_own[0:heads, :] = mm(q_ref[...], place_q)
    qslots[sp] = q_own[...]

    lead = heads // 2
    bit0 = sp % 2

    def actual(i):
        return (i + (1 - bit0) * lead) % heads if heads > 1 else i

    finc8[...] = jnp.zeros_like(finc8)
    for i in range(heads):
        finc8[i : i + 1, :] = finc_ref[pl.ds(actual(i), 1), :]

    total_heads = wb.shape[0]
    row_id = lax.broadcasted_iota(jnp.int32, (LANES, total_heads), 0)
    col_id = lax.broadcasted_iota(jnp.int32, (LANES, total_heads), 1)
    first_head = tp * heads
    shift = (1 - bit0) * lead
    own_head = first_head + (row_id % SUB + shift) % heads
    own = (row_id % SUB < heads) & (col_id == own_head)
    pick_b = jnp.where(own & (row_id < SUB), 1.0, 0.0)
    pick_d = jnp.where(own & (row_id >= SUB) & (row_id < 2 * SUB), 1.0, 0.0)
    loads[2].wait()
    loads[3].wait()
    depth = wg.shape[0]
    piece = 512

    def pick(step, carry):
        rows = pl.ds(pl.multiple_of(step * piece, piece), piece)
        both = mm(pick_b, wb[:, rows]) + mm(pick_d, wd[:, rows])
        wg[rows, :] = jnp.transpose(both).astype(BF16)
        return carry

    lax.fori_loop(0, depth // piece, pick, 0)
    loads[0].wait()
    loads[1].wait()

    def project(x, source, rows, first=False, start=0, size=features):
        deep = pl.ds(pl.multiple_of(source * features + start, size), size)
        for acc, weights in ((acck, wk), (accv, wv), (accg, wg)):
            part = jnp.dot(x, weights[deep, :], preferred_element_type=F32)
            acc[rows, :] = part if first else acc[rows, :] + part

    half_rows = 256 if tokens_here % 256 == 0 else CHUNK

    def own_project(step, carry):
        rows = pl.ds(pl.multiple_of(step * half_rows, half_rows), half_rows)
        project(x_ref[rows, :], tp, rows, True)
        return carry

    lax.fori_loop(0, tokens_here // half_rows, own_project, 0)
    for k in range(parts):
        arrived(sibling, k)

    def sibling_project(step, carry):
        rows = pl.ds(pl.multiple_of(step * half_rows, half_rows), half_rows)
        project(xg[sibling, rows, :], sibling, rows)
        return carry

    lax.fori_loop(0, tokens_here // half_rows, sibling_project, 0)

    row8 = lax.broadcasted_iota(jnp.int32, (SUB, total_heads), 0)
    lane8 = lax.broadcasted_iota(jnp.int32, (SUB, total_heads), 1)
    mine = (lane8 == first_head + (row8 + shift) % heads) & (row8 < heads)
    bias_col = jnp.sum(jnp.where(mine, bias_ref[...], 0.0), axis=1, keepdims=True)
    rate_col = jnp.sum(jnp.where(mine, rate_ref[...], 0.0), axis=1, keepdims=True)

    maps[...] = jnp.zeros_like(maps)
    gams[...] = jnp.ones_like(gams)

    def near(step):
        return ((y + n_y - step) % n_y) * 2 + core

    def far(step):
        return ((y + n_y - step) % n_y) * 2 + 1 - core

    def gate_terms(rows):
        ri = lax.broadcasted_iota(jnp.int32, (CHUNK, CHUNK), 0)
        ci = lax.broadcasted_iota(jnp.int32, (CHUNK, CHUNK), 1)
        strict = ri > ci
        upper = jnp.where(ri <= ci, 1.0, 0.0)
        gates = jnp.transpose(accg[rows, :])
        beta = jax.nn.sigmoid(gates[0:SUB, :] + bias_col)
        raw = gates[SUB : 2 * SUB, :]
        softplus = jnp.maximum(raw, 0.0) + jnp.log1p(jnp.exp(-jnp.abs(raw)))
        logd = -rate_col * softplus + finc8[:, rows]
        cum = jnp.dot(logd, upper, precision=lax.Precision.HIGHEST, preferred_element_type=F32)
        total = jnp.sum(logd, axis=1, keepdims=True)
        columns = jnp.transpose(
            jnp.concatenate(
                [
                    beta,
                    cum,
                    jnp.exp(cum),
                    jnp.exp(total - cum),
                    jnp.zeros((LANES - 4 * SUB, LANES), F32),
                ],
                axis=0,
            )
        )
        return strict, cum, columns, jnp.exp(total)

    def advance(rows, terms, chosen):
        strict, cum, columns, keep = terms
        rights, powers, remains = [], [], []
        for h in chosen:
            cols = pl.ds(pl.multiple_of(actual(h) * DK, DK), DK)
            key = acck[rows, cols].astype(BF16).astype(F32)
            key = key * lax.rsqrt(jnp.sum(key * key, axis=-1, keepdims=True) + norm_eps)
            value = accv[rows, cols].astype(BF16).astype(F32)
            b_col = columns[:, h : h + 1]
            c_col = columns[:, SUB + h : SUB + h + 1]
            e_col = columns[:, 2 * SUB + h : 2 * SUB + h + 1]
            r_col = columns[:, 3 * SUB + h : 3 * SUB + h + 1]
            key_beta = key * b_col
            decay = jnp.exp(jnp.where(strict, c_col - cum[h : h + 1, :], 0.0))
            powers.append(jnp.where(strict, mm_nt(key_beta, key) * decay, 0.0))
            rights.append(jnp.concatenate([value * b_col, key_beta * e_col], axis=1))
            remains.append(jnp.transpose(key * r_col))
        solved = [right - mm(power, right) for power, right in zip(powers, rights)]
        covered = 2
        while covered < CHUNK:
            powers = [mm(power, power) for power in powers]
            solved = [known + mm(power, known) for power, known in zip(powers, solved)]
            covered *= 2
        fresh = []
        for h, known in zip(chosen, solved):
            gamma = gams[h, 0:1, 0:1]
            erase = known[:, DV:]
            direct = jnp.concatenate([known[:, :DV], -gamma * erase], axis=1)
            fresh.append(direct - mm(erase, maps[h]))
        for h, remain, new in zip(chosen, remains, fresh):
            maps[h] = keep[h : h + 1, 0:1] * maps[h] + mm(remain, new)
            gams[h] = keep[h : h + 1, 0:1] * gams[h]

    def chunk_step(c, carry):
        rows = pl.ds(pl.multiple_of(c * CHUNK, CHUNK), CHUNK)
        for step in range(1, n_y):
            arrived(near(step), c)
            copy_forward(step, c).start()
        for step in range(1, n_y):
            project(xg[near(step), rows, :], near(step), rows)
        for step in range(1, n_y):
            arrived(far(step), c)
            project(xg[far(step), rows, :], far(step), rows)
        advance(rows, gate_terms(rows), range(heads))
        return carry

    lax.fori_loop(0, last, chunk_step, 0)

    def far_part(k):
        rows, cols = part_of(k)
        for step in range(1, n_y):
            arrived(far(step), k)
            project(xg[far(step), rows, cols], far(step), rows, False, (k - last) * wide, wide)

    end_rows = pl.ds(last * CHUNK, CHUNK)
    for k in range(last, parts):
        rows, cols = part_of(k)
        for step in range(1, n_y):
            arrived(near(step), k)
            copy_forward(step, k).start()
        for step in range(1, n_y):
            project(xg[near(step), rows, cols], near(step), rows, False, (k - last) * wide, wide)
        if k > last:
            far_part(k - 1)
    far_part(parts - 1)
    end_terms = gate_terms(end_rows)

    count = heads
    offset = 0
    held = 0
    for level in range(levels):
        bit = (sp // (1 << level)) % 2
        partner = flip(1 << level)
        split = count > 1
        half = count // 2 if split else count
        if level == 0:
            send_at, keep_at = 0, heads - half
            advance(end_rows, end_terms, range(half))
        else:
            keep_at = held + (bit * half if split else 0)
            send_at = held + ((1 - bit) * half if split else 0)
        rows = pl.ds(offset, half)
        known_q = pl.ds(sp - sp % (1 << level), 1 << level)
        move_q = pltpu.make_async_remote_copy(
            src_ref=qslots.at[known_q],
            dst_ref=qslots.at[known_q],
            send_sem=q_send.at[level],
            recv_sem=q_recv.at[level],
            device_id={"sp": partner},
            device_id_type=MESH,
        )
        for i in range(half):
            sendbuf[offset + i] = maps[send_at + i].astype(BF16)
            gsend[offset + i] = gams[send_at + i]
        move = pltpu.make_async_remote_copy(
            src_ref=sendbuf.at[rows],
            dst_ref=recvbuf.at[rows],
            send_sem=map_send.at[level],
            recv_sem=map_recv.at[level],
            device_id={"sp": partner},
            device_id_type=MESH,
        )
        move_g = pltpu.make_async_remote_copy(
            src_ref=gsend.at[rows],
            dst_ref=grecv.at[rows],
            send_sem=g_send.at[level],
            recv_sem=g_recv.at[level],
            device_id={"sp": partner},
            device_id_type=MESH,
        )
        move.start()
        move_g.start()
        move_q.start()
        if level == 0 and split:
            advance(end_rows, end_terms, range(half, heads))
        move.wait()
        move_g.wait()
        move_q.wait()
        later = bit == 1
        for i in range(half):
            own = maps[keep_at + i]
            if not split:
                own = own.astype(BF16).astype(F32)
            own_g = gams[keep_at + i]
            got = recvbuf[offset + i].astype(F32)
            got_g = grecv[offset + i]
            left = jnp.where(later, own, got)
            left_g = jnp.where(later, own_g, got_g)
            right = jnp.where(later, got, own)
            right_g = jnp.where(later, got_g, own_g)
            tail = left[:, DV:]
            added = jnp.concatenate([left[:, :DV], right_g[0:1, 0:1] * tail], axis=1)
            maps[keep_at + i] = left_g[0:1, 0:1] * right + mm(tail, right) + added
            gams[keep_at + i] = left_g * right_g
        offset += half
        count = half
        held = keep_at

    my_head = bit0 * lead + held - lead if heads > 1 else 0
    final = maps[held][:, :DV]
    for j in range(n_sp):
        fstate[j] = final[j * rows_out : (j + 1) * rows_out, :].astype(BF16)

    def head_of(index):
        found = 0
        for place in range(log2(heads)):
            found = found * 2 + (index // (1 << place)) % 2
        return found

    def copy_state(step):
        target = flip(step)
        return pltpu.make_async_remote_copy(
            src_ref=fstate.at[target],
            dst_ref=srecv.at[my_head],
            send_sem=s_send.at[step],
            recv_sem=s_recv.at[my_head],
            device_id={"sp": target},
            device_id_type=MESH,
        )

    for step in range(1, heads):
        copy_state(step).start()
    srecv[my_head] = fstate[sp]

    query = jnp.sum(qslots[...], axis=0)
    reads = mm(query, final)
    row_head = lax.broadcasted_iota(jnp.int32, (SUB, DV), 0)
    raw_read = jnp.sum(jnp.where(row_head == my_head, reads, 0.0), axis=0, keepdims=True)
    read = (
        raw_read
        * lax.rsqrt(jnp.mean(raw_read * raw_read, axis=-1, keepdims=True) + norm_eps)
        * gain_ref[...].astype(F32)
    )
    fread[...] = jnp.broadcast_to(read, fread.shape)

    def copy_read(step):
        target = flip(step)
        return pltpu.make_async_remote_copy(
            src_ref=fread,
            dst_ref=rrecv.at[my_head],
            send_sem=r_send.at[step],
            recv_sem=r_recv.at[my_head],
            device_id={"sp": target},
            device_id_type=MESH,
        )

    for step in range(1, heads):
        copy_read(step).start()
    rrecv[my_head] = fread[...]

    for step in range(1, heads):
        source = flip(step)
        head = head_of(source)
        pltpu.make_async_remote_copy(
            src_ref=fstate.at[source],
            dst_ref=srecv.at[head],
            send_sem=s_send.at[step],
            recv_sem=s_recv.at[head],
            device_id={"sp": source},
            device_id_type=MESH,
        ).wait_recv()
        pltpu.make_async_remote_copy(
            src_ref=fread,
            dst_ref=rrecv.at[head],
            send_sem=r_send.at[step],
            recv_sem=r_recv.at[head],
            device_id={"sp": source},
            device_id_type=MESH,
        ).wait_recv()
    for h in range(heads):
        state_out[h] = srecv[h]
        read_out[h : h + 1, :] = rrecv[h, 0:1, :]

    for k in range(parts):
        copy_own(k).wait_send()
        for step in range(1, n_y):
            copy_peer(step, k).wait_send()
            copy_forward(step, k).wait_send()
    for step in range(1, heads):
        copy_state(step).wait_send()
        copy_read(step).wait_send()


def per_device(
    n_sp,
    n_tp,
    tokens,
    w_key,
    w_value,
    w_beta,
    w_decay,
    beta_bias,
    decay_rate,
    forgetting_increment,
    new_query,
    read_gain,
):
    tokens_here, features = tokens.shape
    depth, width = w_key.shape
    heads = width // DK
    parts = tokens_here // CHUNK - 1 + tail_pieces(features)
    rows_out = DK // n_sp
    n_y = n_tp // 2
    levels = log2(n_sp)
    slots = 0
    count = heads
    for _ in range(levels):
        count = max(count // 2, 1)
        slots += count
    vmem = pl.BlockSpec(memory_space=pltpu.VMEM)
    hbm = pl.BlockSpec(memory_space=pl.ANY)
    dma = pltpu.SemaphoreType.DMA
    return pl.pallas_call(
        functools.partial(body, n_sp, n_tp),
        name="delta_state",
        out_shape=(
            jax.ShapeDtypeStruct((heads, rows_out, DV), BF16),
            jax.ShapeDtypeStruct((heads, DV), F32),
        ),
        in_specs=[hbm, hbm, hbm, hbm, hbm, vmem, vmem, vmem, vmem, vmem],
        out_specs=(vmem, vmem),
        scratch_shapes=[
            pltpu.VMEM((depth, width), BF16),
            pltpu.VMEM((depth, width), BF16),
            pltpu.VMEM(w_beta.shape[::-1], BF16),
            pltpu.VMEM(w_decay.shape[::-1], BF16),
            pltpu.VMEM((depth, LANES), BF16),
            pltpu.VMEM((tokens_here, features), BF16),
            pltpu.VMEM((SUB, tokens_here), F32),
            pltpu.VMEM((SUB, DK), F32),
            pltpu.VMEM((n_tp, tokens_here, features), BF16),
            pltpu.VMEM((tokens_here, width), F32),
            pltpu.VMEM((tokens_here, width), F32),
            pltpu.VMEM((tokens_here, LANES), F32),
            pltpu.VMEM((heads, DK, DV + DK), F32),
            pltpu.VMEM((heads, SUB, LANES), F32),
            pltpu.VMEM((slots, DK, DV + DK), BF16),
            pltpu.VMEM((slots, DK, DV + DK), BF16),
            pltpu.VMEM((slots, SUB, LANES), F32),
            pltpu.VMEM((slots, SUB, LANES), F32),
            pltpu.VMEM((n_sp, SUB, DK), F32),
            pltpu.VMEM((n_sp, rows_out, DV), BF16),
            pltpu.VMEM((heads, rows_out, DV), BF16),
            pltpu.VMEM((SUB, DV), F32),
            pltpu.VMEM((heads, SUB, DV), F32),
            dma((5,)),
            dma((parts,)),
            dma((n_y, parts)),
            dma((n_y, parts)),
            dma((n_tp, parts)),
            dma((levels,)),
            dma((levels,)),
            dma((levels,)),
            dma((levels,)),
            dma((levels,)),
            dma((levels,)),
            dma((heads,)),
            dma((heads,)),
            dma((heads,)),
            dma((heads,)),
        ],
        compiler_params=pltpu.CompilerParams(
            collective_id=0, has_side_effects=True, vmem_limit_bytes=60 * 1024 * 1024
        ),
    )(
        tokens,
        w_key,
        w_value,
        w_beta.T,
        w_decay.T,
        beta_bias[None, :],
        decay_rate[None, :],
        forgetting_increment,
        new_query,
        read_gain[None, :],
    )


def solution(mesh):
    return jax.shard_map(
        functools.partial(per_device, mesh.shape["sp"], mesh.shape["tp"]),
        mesh=mesh,
        in_specs=(
            P("sp", "tp"),
            P(None, "tp"),
            P(None, "tp"),
            P(),
            P(),
            P(),
            P(),
            P("tp", "sp"),
            P("tp", "sp"),
            P(),
        ),
        out_specs=(P("tp", "sp", None), P("tp", None)),
        check_vma=False,
    )
```

```python
import functools

import jax
import jax.numpy as jnp
from jax import lax
from jax.experimental import pallas as pl
from jax.experimental.pallas import tpu as pltpu
from jax.sharding import PartitionSpec as P

DK = 128
DV = 128
CHUNK = 128
LANES = 128
SUB = 8
norm_eps = 1e-06
MESH = pl.DeviceIdType.MESH
F32 = jnp.float32
BF16 = jnp.bfloat16


def mm(left, right):
    return jnp.dot(left.astype(BF16), right.astype(BF16), preferred_element_type=F32)


def mm_nt(left, right):
    return lax.dot_general(
        left.astype(BF16), right.astype(BF16), (((1,), (1,)), ((), ())), preferred_element_type=F32
    )


def log2(value):
    return value.bit_length() - 1


def tail_pieces(features):
    return 4 if features % 1024 == 0 else 1


def body(
    n_sp,
    n_tp,
    x_hbm,
    wk_hbm,
    wv_hbm,
    wb_hbm,
    wd_hbm,
    bias_ref,
    rate_ref,
    finc_ref,
    q_ref,
    gain_ref,
    state_out,
    read_out,
    wk,
    wv,
    wb,
    wd,
    wg,
    x_ref,
    finc8,
    q_own,
    xg,
    acck,
    accv,
    accg,
    maps,
    gams,
    sendbuf,
    recvbuf,
    gsend,
    grecv,
    qslots,
    fstate,
    srecv,
    fread,
    rrecv,
    wsem,
    own_send,
    peer_send,
    fwd_send,
    tok_recv,
    q_send,
    q_recv,
    map_send,
    map_recv,
    g_send,
    g_recv,
    s_send,
    s_recv,
    r_send,
    r_recv,
):
    sp = lax.axis_index("sp")
    tp = lax.axis_index("tp")
    tokens_here, features = x_ref.shape
    heads = wk.shape[1] // DK
    chunks = tokens_here // CHUNK
    last = chunks - 1
    pieces = tail_pieces(features)
    wide = features // pieces
    parts = last + pieces
    n_y = n_tp // 2
    y = tp // 2
    core = tp % 2
    sibling = tp + 1 - 2 * core
    levels = log2(n_sp)
    rows_out = DK // n_sp

    load_x = pltpu.make_async_copy(x_hbm, x_ref, wsem.at[4])
    load_x.start()
    loads = [
        pltpu.make_async_copy(wk_hbm, wk, wsem.at[0]),
        pltpu.make_async_copy(wv_hbm, wv, wsem.at[1]),
        pltpu.make_async_copy(wb_hbm, wb, wsem.at[2]),
        pltpu.make_async_copy(wd_hbm, wd, wsem.at[3]),
    ]
    for load in (loads[2], loads[3], loads[0], loads[1]):
        load.start()

    barrier = pltpu.get_barrier_semaphore()
    pl.semaphore_signal(barrier, inc=1, device_id={"tp": sibling}, device_id_type=MESH)
    for step in range(1, n_y):
        peer = ((y + step) % n_y) * 2 + core
        pl.semaphore_signal(barrier, inc=1, device_id={"tp": peer}, device_id_type=MESH)
    masks = sorted(set(range(1, heads)) | {1 << level for level in range(levels)})

    def flip(mask):
        found = sp
        for place in range(levels):
            if (mask >> place) % 2:
                found = found + (1 - 2 * ((sp // (1 << place)) % 2)) * (1 << place)
        return found

    for mask in masks:
        pl.semaphore_signal(barrier, inc=1, device_id={"sp": flip(mask)}, device_id_type=MESH)

    def part_of(k):
        if isinstance(k, int) and k >= last:
            return pl.ds(last * CHUNK, CHUNK), pl.ds((k - last) * wide, wide)
        start = k * CHUNK if isinstance(k, int) else pl.multiple_of(k * CHUNK, CHUNK)
        return pl.ds(start, CHUNK), pl.ds(0, features)

    def copy_own(k):
        rows, cols = part_of(k)
        return pltpu.make_async_remote_copy(
            src_ref=x_ref.at[rows, cols],
            dst_ref=xg.at[tp, rows, cols],
            send_sem=own_send.at[k],
            recv_sem=tok_recv.at[tp, k],
            device_id={"tp": sibling},
            device_id_type=MESH,
        )

    def copy_peer(step, k):
        rows, cols = part_of(k)
        peer = ((y + step) % n_y) * 2 + core
        return pltpu.make_async_remote_copy(
            src_ref=x_ref.at[rows, cols],
            dst_ref=xg.at[tp, rows, cols],
            send_sem=peer_send.at[step, k],
            recv_sem=tok_recv.at[tp, k],
            device_id={"tp": peer},
            device_id_type=MESH,
        )

    def copy_forward(step, k):
        rows, cols = part_of(k)
        source = ((y + n_y - step) % n_y) * 2 + core
        return pltpu.make_async_remote_copy(
            src_ref=xg.at[source, rows, cols],
            dst_ref=xg.at[source, rows, cols],
            send_sem=fwd_send.at[step, k],
            recv_sem=tok_recv.at[source, k],
            device_id={"tp": sibling},
            device_id_type=MESH,
        )

    def arrived(source, k):
        rows, cols = part_of(k)
        pltpu.make_async_remote_copy(
            src_ref=xg.at[source, rows, cols],
            dst_ref=xg.at[source, rows, cols],
            send_sem=own_send.at[k],
            recv_sem=tok_recv.at[source, k],
            device_id={"tp": sibling},
            device_id_type=MESH,
        ).wait_recv()

    pl.semaphore_wait(barrier, n_y + len(masks))
    load_x.wait()
    for k in range(parts):
        for step in range(1, n_y):
            copy_peer(step, k).start()
        copy_own(k).start()

    rows_q = lax.broadcasted_iota(jnp.int32, (rows_out, LANES), 0)
    lanes_q = lax.broadcasted_iota(jnp.int32, (rows_out, LANES), 1)
    place_q = jnp.where(lanes_q == rows_q + sp * rows_out, 1.0, 0.0)
    q_own[...] = jnp.zeros_like(q_own)
    q_own[0:heads, :] = mm(q_ref[...], place_q)
    qslots[sp] = q_own[...]

    lead = heads // 2
    bit0 = sp % 2

    def actual(i):
        return (i + (1 - bit0) * lead) % heads if heads > 1 else i

    finc8[...] = jnp.zeros_like(finc8)
    for i in range(heads):
        finc8[i : i + 1, :] = finc_ref[pl.ds(actual(i), 1), :]

    total_heads = wb.shape[0]
    row_id = lax.broadcasted_iota(jnp.int32, (LANES, total_heads), 0)
    col_id = lax.broadcasted_iota(jnp.int32, (LANES, total_heads), 1)
    first_head = tp * heads
    shift = (1 - bit0) * lead
    own_head = first_head + (row_id % SUB + shift) % heads
    own = (row_id % SUB < heads) & (col_id == own_head)
    pick_b = jnp.where(own & (row_id < SUB), 1.0, 0.0)
    pick_d = jnp.where(own & (row_id >= SUB) & (row_id < 2 * SUB), 1.0, 0.0)
    loads[2].wait()
    loads[3].wait()
    depth = wg.shape[0]
    piece = 512

    def pick(step, carry):
        rows = pl.ds(pl.multiple_of(step * piece, piece), piece)
        both = mm(pick_b, wb[:, rows]) + mm(pick_d, wd[:, rows])
        wg[rows, :] = jnp.transpose(both).astype(BF16)
        return carry

    lax.fori_loop(0, depth // piece, pick, 0)
    loads[0].wait()
    loads[1].wait()

    def project(x, source, rows, first=False, start=0, size=features):
        deep = pl.ds(pl.multiple_of(source * features + start, size), size)
        for acc, weights in ((acck, wk), (accv, wv), (accg, wg)):
            part = jnp.dot(x, weights[deep, :], preferred_element_type=F32)
            acc[rows, :] = part if first else acc[rows, :] + part

    half_rows = 256 if tokens_here % 256 == 0 else CHUNK

    def own_project(step, carry):
        rows = pl.ds(pl.multiple_of(step * half_rows, half_rows), half_rows)
        project(x_ref[rows, :], tp, rows, True)
        return carry

    lax.fori_loop(0, tokens_here // half_rows, own_project, 0)
    for k in range(parts):
        arrived(sibling, k)

    def sibling_project(step, carry):
        rows = pl.ds(pl.multiple_of(step * half_rows, half_rows), half_rows)
        project(xg[sibling, rows, :], sibling, rows)
        return carry

    lax.fori_loop(0, tokens_here // half_rows, sibling_project, 0)

    row8 = lax.broadcasted_iota(jnp.int32, (SUB, total_heads), 0)
    lane8 = lax.broadcasted_iota(jnp.int32, (SUB, total_heads), 1)
    mine = (lane8 == first_head + (row8 + shift) % heads) & (row8 < heads)
    bias_col = jnp.sum(jnp.where(mine, bias_ref[...], 0.0), axis=1, keepdims=True)
    rate_col = jnp.sum(jnp.where(mine, rate_ref[...], 0.0), axis=1, keepdims=True)

    maps[...] = jnp.zeros_like(maps)
    gams[...] = jnp.ones_like(gams)

    def near(step):
        return ((y + n_y - step) % n_y) * 2 + core

    def far(step):
        return ((y + n_y - step) % n_y) * 2 + 1 - core

    def gate_terms(rows):
        ri = lax.broadcasted_iota(jnp.int32, (CHUNK, CHUNK), 0)
        ci = lax.broadcasted_iota(jnp.int32, (CHUNK, CHUNK), 1)
        strict = ri > ci
        upper = jnp.where(ri <= ci, 1.0, 0.0)
        gates = jnp.transpose(accg[rows, :])
        beta = jax.nn.sigmoid(gates[0:SUB, :] + bias_col)
        raw = gates[SUB : 2 * SUB, :]
        softplus = jnp.maximum(raw, 0.0) + jnp.log1p(jnp.exp(-jnp.abs(raw)))
        logd = -rate_col * softplus + finc8[:, rows]
        cum = jnp.dot(logd, upper, precision=lax.Precision.HIGHEST, preferred_element_type=F32)
        total = jnp.sum(logd, axis=1, keepdims=True)
        columns = jnp.transpose(
            jnp.concatenate(
                [
                    beta,
                    cum,
                    jnp.exp(cum),
                    jnp.exp(total - cum),
                    jnp.zeros((LANES - 4 * SUB, LANES), F32),
                ],
                axis=0,
            )
        )
        return strict, cum, columns, jnp.exp(total)

    def advance(rows, terms, chosen):
        strict, cum, columns, keep = terms
        rights, powers, remains = [], [], []
        for h in chosen:
            cols = pl.ds(pl.multiple_of(actual(h) * DK, DK), DK)
            key = acck[rows, cols].astype(BF16).astype(F32)
            key = key * lax.rsqrt(jnp.sum(key * key, axis=-1, keepdims=True) + norm_eps)
            value = accv[rows, cols].astype(BF16).astype(F32)
            b_col = columns[:, h : h + 1]
            c_col = columns[:, SUB + h : SUB + h + 1]
            e_col = columns[:, 2 * SUB + h : 2 * SUB + h + 1]
            r_col = columns[:, 3 * SUB + h : 3 * SUB + h + 1]
            key_beta = key * b_col
            decay = jnp.exp(jnp.where(strict, c_col - cum[h : h + 1, :], 0.0))
            powers.append(jnp.where(strict, mm_nt(key_beta, key) * decay, 0.0))
            rights.append(jnp.concatenate([value * b_col, key_beta * e_col], axis=1))
            remains.append(jnp.transpose(key * r_col))
        solved = [right - mm(power, right) for power, right in zip(powers, rights)]
        covered = 2
        while covered < CHUNK:
            powers = [mm(power, power) for power in powers]
            solved = [known + mm(power, known) for power, known in zip(powers, solved)]
            covered *= 2
        fresh = []
        for h, known in zip(chosen, solved):
            gamma = gams[h, 0:1, 0:1]
            erase = known[:, DV:]
            direct = jnp.concatenate([known[:, :DV], -gamma * erase], axis=1)
            fresh.append(direct - mm(erase, maps[h]))
        for h, remain, new in zip(chosen, remains, fresh):
            maps[h] = keep[h : h + 1, 0:1] * maps[h] + mm(remain, new)
            gams[h] = keep[h : h + 1, 0:1] * gams[h]

    def chunk_step(c, carry):
        rows = pl.ds(pl.multiple_of(c * CHUNK, CHUNK), CHUNK)
        for step in range(1, n_y):
            arrived(near(step), c)
            copy_forward(step, c).start()
        for step in range(1, n_y):
            project(xg[near(step), rows, :], near(step), rows)
        for step in range(1, n_y):
            arrived(far(step), c)
            project(xg[far(step), rows, :], far(step), rows)
        advance(rows, gate_terms(rows), range(heads))
        return carry

    lax.fori_loop(0, last, chunk_step, 0)

    def far_part(k):
        rows, cols = part_of(k)
        for step in range(1, n_y):
            arrived(far(step), k)
            project(xg[far(step), rows, cols], far(step), rows, False, (k - last) * wide, wide)

    end_rows = pl.ds(last * CHUNK, CHUNK)
    for k in range(last, parts):
        rows, cols = part_of(k)
        for step in range(1, n_y):
            arrived(near(step), k)
            copy_forward(step, k).start()
        for step in range(1, n_y):
            project(xg[near(step), rows, cols], near(step), rows, False, (k - last) * wide, wide)
        if k > last:
            far_part(k - 1)
    far_part(parts - 1)
    end_terms = gate_terms(end_rows)

    count = heads
    offset = 0
    held = 0
    for level in range(levels):
        bit = (sp // (1 << level)) % 2
        partner = flip(1 << level)
        split = count > 1
        half = count // 2 if split else count
        if level == 0:
            send_at, keep_at = 0, heads - half
            advance(end_rows, end_terms, range(half))
        else:
            keep_at = held + (bit * half if split else 0)
            send_at = held + ((1 - bit) * half if split else 0)
        rows = pl.ds(offset, half)
        known_q = pl.ds(sp - sp % (1 << level), 1 << level)
        move_q = pltpu.make_async_remote_copy(
            src_ref=qslots.at[known_q],
            dst_ref=qslots.at[known_q],
            send_sem=q_send.at[level],
            recv_sem=q_recv.at[level],
            device_id={"sp": partner},
            device_id_type=MESH,
        )
        for i in range(half):
            sendbuf[offset + i] = maps[send_at + i].astype(BF16)
            gsend[offset + i] = gams[send_at + i]
        move = pltpu.make_async_remote_copy(
            src_ref=sendbuf.at[rows],
            dst_ref=recvbuf.at[rows],
            send_sem=map_send.at[level],
            recv_sem=map_recv.at[level],
            device_id={"sp": partner},
            device_id_type=MESH,
        )
        move_g = pltpu.make_async_remote_copy(
            src_ref=gsend.at[rows],
            dst_ref=grecv.at[rows],
            send_sem=g_send.at[level],
            recv_sem=g_recv.at[level],
            device_id={"sp": partner},
            device_id_type=MESH,
        )
        move.start()
        move_g.start()
        move_q.start()
        if level == 0 and split:
            advance(end_rows, end_terms, range(half, heads))
        move.wait()
        move_g.wait()
        move_q.wait()
        later = bit == 1
        for i in range(half):
            own = maps[keep_at + i]
            if not split:
                own = own.astype(BF16).astype(F32)
            own_g = gams[keep_at + i]
            got = recvbuf[offset + i].astype(F32)
            got_g = grecv[offset + i]
            left = jnp.where(later, own, got)
            left_g = jnp.where(later, own_g, got_g)
            right = jnp.where(later, got, own)
            right_g = jnp.where(later, got_g, own_g)
            tail = left[:, DV:]
            added = jnp.concatenate([left[:, :DV], right_g[0:1, 0:1] * tail], axis=1)
            maps[keep_at + i] = left_g[0:1, 0:1] * right + mm(tail, right) + added
            gams[keep_at + i] = left_g * right_g
        offset += half
        count = half
        held = keep_at

    my_head = bit0 * lead + held - lead if heads > 1 else 0
    final = maps[held][:, :DV]
    for j in range(n_sp):
        fstate[j] = final[j * rows_out : (j + 1) * rows_out, :].astype(BF16)

    def head_of(index):
        found = 0
        for place in range(log2(heads)):
            found = found * 2 + (index // (1 << place)) % 2
        return found

    def copy_state(step):
        target = flip(step)
        return pltpu.make_async_remote_copy(
            src_ref=fstate.at[target],
            dst_ref=srecv.at[my_head],
            send_sem=s_send.at[step],
            recv_sem=s_recv.at[my_head],
            device_id={"sp": target},
            device_id_type=MESH,
        )

    for step in range(1, heads):
        copy_state(step).start()
    srecv[my_head] = fstate[sp]

    query = jnp.sum(qslots[...], axis=0)
    reads = mm(query, final)
    row_head = lax.broadcasted_iota(jnp.int32, (SUB, DV), 0)
    raw_read = jnp.sum(jnp.where(row_head == my_head, reads, 0.0), axis=0, keepdims=True)
    read = (
        raw_read
        * lax.rsqrt(jnp.mean(raw_read * raw_read, axis=-1, keepdims=True) + norm_eps)
        * gain_ref[...].astype(F32)
    )
    fread[...] = jnp.broadcast_to(read, fread.shape)

    def copy_read(step):
        target = flip(step)
        return pltpu.make_async_remote_copy(
            src_ref=fread,
            dst_ref=rrecv.at[my_head],
            send_sem=r_send.at[step],
            recv_sem=r_recv.at[my_head],
            device_id={"sp": target},
            device_id_type=MESH,
        )

    for step in range(1, heads):
        copy_read(step).start()
    rrecv[my_head] = fread[...]

    for step in range(1, heads):
        source = flip(step)
        head = head_of(source)
        pltpu.make_async_remote_copy(
            src_ref=fstate.at[source],
            dst_ref=srecv.at[head],
            send_sem=s_send.at[step],
            recv_sem=s_recv.at[head],
            device_id={"sp": source},
            device_id_type=MESH,
        ).wait_recv()
        pltpu.make_async_remote_copy(
            src_ref=fread,
            dst_ref=rrecv.at[head],
            send_sem=r_send.at[step],
            recv_sem=r_recv.at[head],
            device_id={"sp": source},
            device_id_type=MESH,
        ).wait_recv()
    for h in range(heads):
        state_out[h] = srecv[h]
        read_out[h : h + 1, :] = rrecv[h, 0:1, :]

    for k in range(parts):
        copy_own(k).wait_send()
        for step in range(1, n_y):
            copy_peer(step, k).wait_send()
            copy_forward(step, k).wait_send()
    for step in range(1, heads):
        copy_state(step).wait_send()
        copy_read(step).wait_send()


def hand_over(state_ref, read_ref, state_out, read_out):
    state_out[...] = state_ref[...]
    read_out[...] = read_ref[...]


def per_device(
    n_sp,
    n_tp,
    tokens,
    w_key,
    w_value,
    w_beta,
    w_decay,
    beta_bias,
    decay_rate,
    forgetting_increment,
    new_query,
    read_gain,
):
    tokens_here, features = tokens.shape
    depth, width = w_key.shape
    heads = width // DK
    parts = tokens_here // CHUNK - 1 + tail_pieces(features)
    rows_out = DK // n_sp
    n_y = n_tp // 2
    levels = log2(n_sp)
    slots = 0
    count = heads
    for _ in range(levels):
        count = max(count // 2, 1)
        slots += count
    vmem = pl.BlockSpec(memory_space=pltpu.VMEM)
    hbm = pl.BlockSpec(memory_space=pl.ANY)
    dma = pltpu.SemaphoreType.DMA
    state, read = pl.pallas_call(
        functools.partial(body, n_sp, n_tp),
        name="delta_state",
        out_shape=(
            jax.ShapeDtypeStruct((heads, rows_out, DV), BF16),
            jax.ShapeDtypeStruct((heads, DV), F32),
        ),
        in_specs=[hbm, hbm, hbm, hbm, hbm, vmem, vmem, vmem, vmem, vmem],
        out_specs=(vmem, vmem),
        scratch_shapes=[
            pltpu.VMEM((depth, width), BF16),
            pltpu.VMEM((depth, width), BF16),
            pltpu.VMEM(w_beta.shape[::-1], BF16),
            pltpu.VMEM(w_decay.shape[::-1], BF16),
            pltpu.VMEM((depth, LANES), BF16),
            pltpu.VMEM((tokens_here, features), BF16),
            pltpu.VMEM((SUB, tokens_here), F32),
            pltpu.VMEM((SUB, DK), F32),
            pltpu.VMEM((n_tp, tokens_here, features), BF16),
            pltpu.VMEM((tokens_here, width), F32),
            pltpu.VMEM((tokens_here, width), F32),
            pltpu.VMEM((tokens_here, LANES), F32),
            pltpu.VMEM((heads, DK, DV + DK), F32),
            pltpu.VMEM((heads, SUB, LANES), F32),
            pltpu.VMEM((slots, DK, DV + DK), BF16),
            pltpu.VMEM((slots, DK, DV + DK), BF16),
            pltpu.VMEM((slots, SUB, LANES), F32),
            pltpu.VMEM((slots, SUB, LANES), F32),
            pltpu.VMEM((n_sp, SUB, DK), F32),
            pltpu.VMEM((n_sp, rows_out, DV), BF16),
            pltpu.VMEM((heads, rows_out, DV), BF16),
            pltpu.VMEM((SUB, DV), F32),
            pltpu.VMEM((heads, SUB, DV), F32),
            dma((5,)),
            dma((parts,)),
            dma((n_y, parts)),
            dma((n_y, parts)),
            dma((n_tp, parts)),
            dma((levels,)),
            dma((levels,)),
            dma((levels,)),
            dma((levels,)),
            dma((levels,)),
            dma((levels,)),
            dma((heads,)),
            dma((heads,)),
            dma((heads,)),
            dma((heads,)),
        ],
        compiler_params=pltpu.CompilerParams(
            collective_id=0, has_side_effects=True, vmem_limit_bytes=60 * 1024 * 1024
        ),
    )(
        tokens,
        w_key,
        w_value,
        w_beta.T,
        w_decay.T,
        beta_bias[None, :],
        decay_rate[None, :],
        forgetting_increment,
        new_query,
        read_gain[None, :],
    )
    return pl.pallas_call(
        hand_over,
        name="hand_over",
        out_shape=(
            jax.ShapeDtypeStruct(state.shape, state.dtype),
            jax.ShapeDtypeStruct(read.shape, read.dtype),
        ),
        in_specs=[vmem, vmem],
        out_specs=(vmem, vmem),
    )(state, read)


def solution(mesh):
    return jax.shard_map(
        functools.partial(per_device, mesh.shape["sp"], mesh.shape["tp"]),
        mesh=mesh,
        in_specs=(
            P("sp", "tp"),
            P(None, "tp"),
            P(None, "tp"),
            P(),
            P(),
            P(),
            P(),
            P("tp", "sp"),
            P("tp", "sp"),
            P(),
        ),
        out_specs=(P("tp", "sp", None), P("tp", None)),
        check_vma=False,
    )
```
